256 devices in a mesh: gr: 2 (over z_hi), sp: 16 (over z_lo, y), tp: 8 (over x, core).
Axes of the slice: x: 4, y: 4, z: 8 (z_hi: 2, z_lo: 4; z = z_hi * 4 + z_lo), core: 2. Of those that a mesh axis runs over, the one named last changes fastest.
Arguments:
- tokens: bfloat16 [8, 3072, 4096], P('gr', 'sp', 'tp'), may hold values from -6.5 to 6.5
- first_token_input: bfloat16 [8, 4096], P('gr', 'sp'), may hold values from -6 to 6
- forget_weight: bfloat16 [4096, 4096], P(None, 'tp'), may hold values from -0.1171875 to 0.1171875
- value_weight: bfloat16 [4096, 4096], P(None, 'tp'), may hold values from -0.375 to 0.375
- query_weight: bfloat16 [4096, 4096], P('sp', 'tp'), may hold values from -0.09375 to 0.09375
- output_gate_weight: bfloat16 [4096, 4096], P('sp', 'tp'), may hold values from -0.09375 to 0.09375
- forget_bound_slack: float32 [4096], P('tp'), may hold values from 0.00016276042 to 0.8, as said below
- additional_damping_exponent: float32 [8, 3072, 32], P('gr', 'sp', 'tp'), may hold values from -2.2 to 0, as said below
- read_norm_scale: float32 [128], replicated, may hold values from 0.1 to 1.9
Outputs:
- cache: bfloat16 [8, 32, 128, 128], P('gr', 'tp', 'sp')
- first_read: bfloat16 [8, 4096], P('gr', 'tp')
The draws below stay inside these ranges and needn't reach their ends.
Inputs may be any that keep to these rules, and one draw needn't show every extreme that they name: `forget_bound_slack`: positive gaps, one per channel. `additional_damping_exponent`: non-positive log-decays.
All inputs are finite; a program needn't handle non-finite values.
Results may differ from the reference program's by a relative error of at most 0.018.
Values may be sent and summed in bfloat16 or wider, within the bound.
A program may use at most 64 MiB of HBM per device.

```python
import math
import jax
import jax.numpy as jnp
from jax import lax

D = 4096
HEADS = 32
ATTENTION_SPAN = 128
HW = 4096
LEN = 3072
SEQS_ALL = 8


def shared_direction(key):
    signs = jax.random.randint(jax.random.fold_in(key, 101), (D,), 0, 2)
    return (signs * 2 - 1).astype(jnp.float32)


def draw_tokens(key, part):
    direction = shared_direction(key)
    base_key, coef_key = jax.random.split(jax.random.fold_in(key, 31))
    base = jnp.clip(jax.random.normal(base_key, (SEQS_ALL, LEN, D), jnp.float32), -6.0, 6.0)
    coef = jax.random.uniform(coef_key, (SEQS_ALL, 16, 1), jnp.float32, 0.0, 1.5)
    coef = jnp.repeat(coef, LEN // 16, axis=1)
    return (base + coef * 0.3 * direction[None, None, :]).astype(jnp.bfloat16)


def draw_forget_weight(key, part):
    direction = shared_direction(key)
    base_key = jax.random.fold_in(key, 43)
    spread = 1.0 / math.sqrt(D)
    base = jnp.clip(jax.random.normal(base_key, (D, HW), jnp.float32), -6.0, 6.0) * spread
    return (base + 11.0 / D * direction[:, None]).astype(jnp.bfloat16)


def draw_forget_bound_slack(key, part):
    heads_key, jitter_key = jax.random.split(jax.random.fold_in(key, 11))
    share = 0.5
    slow = jax.random.uniform(heads_key, (HEADS,), jnp.float32) < share
    quick = min(0.4, max(0.05, 16.0 / LEN))
    base = jnp.where(slow, 1.0 / LEN, quick)
    jitter = jnp.exp(jax.random.uniform(jitter_key, (HEADS, ATTENTION_SPAN), jnp.float32, -0.69, 0.69))
    return (base[:, None] * jitter).reshape(HEADS * ATTENTION_SPAN).astype(jnp.float32)


def draw_additional_damping_exponent(key, part):
    rate_key, place_key, size_key = jax.random.split(jax.random.fold_in(key, 23), 3)
    rates = jnp.exp(jax.random.uniform(rate_key, (SEQS_ALL, 16, HEADS), jnp.float32, math.log(0.1), 0.0)) / LEN
    rates = jnp.repeat(rates, LEN // 16, axis=1)
    places = jax.random.randint(place_key, (SEQS_ALL, 3), 0, LEN)
    positions = jnp.arange(LEN, dtype=jnp.int32)
    hits = jnp.sum((positions[None, :, None] == places[:, None, :]).astype(jnp.float32), axis=2)
    strength = jax.random.uniform(size_key, (SEQS_ALL, 1, HEADS), jnp.float32, 0.22, 0.69)
    return (-rates - hits[:, :, None] * strength).astype(jnp.float32)


def block_levels(stream_key, shape, cuts, low, top_value):
    def one(dim, blocks):
        steps = jax.random.uniform(jax.random.fold_in(jax.random.fold_in(stream_key, 6), dim), (blocks,), jnp.float32, low / len(cuts), top_value / len(cuts))
        return jnp.repeat(jnp.exp(steps), shape[dim] // blocks).reshape((-1,) + (1,) * (len(shape) - dim - 1))

    level = one(*cuts[0])
    for cut in cuts[1:]:
        level = level * one(*cut)
    return level


def noise(own_key, shape, width, limit, pieces=(), held_as=jnp.bfloat16):
    result = jax.random.normal(own_key, shape, jnp.float32) * width
    if len(pieces) > 0:
        result = block_levels(own_key, shape, pieces, -0.22, 0.18) * result
    return jnp.clip(result, min=-limit, max=limit).astype(held_as)


def setup_inputs(seed: int = 0) -> dict:
    splits = jax.random.split(jax.random.key(seed), 10)
    return {
        "tokens": draw_tokens(jax.random.fold_in(splits[9], 71), 0),
        "first_token_input": noise(splits[1], (SEQS_ALL, D), 1.0, 6.0, ((0, 2), (1, 16))),
        "forget_weight": draw_forget_weight(jax.random.fold_in(splits[9], 71), 0),
        "value_weight": noise(splits[3], (D, HW), (D // 16) ** -0.5, 0.375, ((1, 8),)),
        "query_weight": noise(splits[4], (D, HW), D ** -0.5, 0.09375, ((0, 16), (1, 8))),
        "output_gate_weight": noise(splits[5], (D, HW), D ** -0.5, 0.09375, ((0, 16), (1, 8))),
        "forget_bound_slack": draw_forget_bound_slack(jax.random.fold_in(splits[9], 71), 0),
        "additional_damping_exponent": draw_additional_damping_exponent(jax.random.fold_in(splits[9], 71), 0),
        "read_norm_scale": jnp.clip(1.0 + 0.18 * jax.random.normal(splits[8], (ATTENTION_SPAN,), jnp.float32), 0.1, 1.9),
    }


def reference(tokens, first_token_input, forget_weight, value_weight, query_weight, output_gate_weight, forget_bound_slack, additional_damping_exponent, read_norm_scale):

    def sequence_wise(couple_bundle):
        series_lines, segment_damping_exponent = couple_bundle
        forget = jnp.dot(series_lines, forget_weight, preferred_element_type=jnp.float32).astype(jnp.bfloat16)
        values = jnp.dot(series_lines, value_weight, preferred_element_type=jnp.float32).astype(jnp.bfloat16)
        valve_sampler_seeds = forget_bound_slack * jax.nn.sigmoid(-forget.astype(jnp.float32))
        damping_exponent = jnp.log1p(-valve_sampler_seeds) + jnp.repeat(segment_damping_exponent, ATTENTION_SPAN, axis=1)
        later_sum = jnp.cumsum(damping_exponent[::-1], axis=0)[::-1] - damping_exponent
        weighted = (valve_sampler_seeds * jnp.exp(later_sum)).astype(jnp.bfloat16)
        key_weights = weighted.astype(jnp.float32).reshape(LEN, HEADS, ATTENTION_SPAN)
        value_rows = values.astype(jnp.float32).reshape(LEN, HEADS, ATTENTION_SPAN)
        return jnp.einsum('lha,lhb->hab', key_weights, value_rows).astype(jnp.bfloat16)
    cache = lax.map(sequence_wise, (tokens, additional_damping_exponent))
    new_query = jnp.dot(first_token_input, query_weight, preferred_element_type=jnp.float32).astype(jnp.bfloat16)
    new_gate = jnp.dot(first_token_input, output_gate_weight, preferred_element_type=jnp.float32).astype(jnp.bfloat16)
    new_forget = jnp.dot(first_token_input, forget_weight, preferred_element_type=jnp.float32).astype(jnp.bfloat16)
    new_value = jnp.dot(first_token_input, value_weight, preferred_element_type=jnp.float32).astype(jnp.bfloat16)
    seq_count = first_token_input.shape[0]
    new_keys = (forget_bound_slack * jax.nn.sigmoid(-new_forget.astype(jnp.float32))).reshape(seq_count, HEADS, ATTENTION_SPAN)
    value_new = new_value.astype(jnp.float32).reshape(seq_count, HEADS, ATTENTION_SPAN)
    updated = (1.0 - new_keys)[..., None] * cache.astype(jnp.float32) + new_keys[..., None] * value_new[:, :, None, :]
    query_rows = new_query.astype(jnp.float32).reshape(seq_count, HEADS, ATTENTION_SPAN)
    read_sum = jnp.einsum('sha,shab->shb', query_rows, updated, precision=lax.Precision.HIGHEST)
    scaled = read_sum * lax.rsqrt(lax.optimization_barrier(jnp.mean(read_sum * read_sum, axis=-1, keepdims=True)) + 1e-06) * read_norm_scale
    first_read = (scaled.reshape(seq_count, HEADS * ATTENTION_SPAN) * jax.nn.silu(new_gate.astype(jnp.float32))).astype(jnp.bfloat16)
    return (cache, first_read)
```

```python
import functools

import jax
import jax.numpy as jnp
from jax import lax
from jax.experimental import pallas as pl
from jax.experimental.pallas import tpu as pltpu
from jax.sharding import PartitionSpec as P

MESH = pl.DeviceIdType.MESH
F32, BF16 = jnp.float32, jnp.bfloat16
AHEAD = 2


def kernel(
    dims,
    tok,
    fti,
    wf,
    wv,
    wq,
    wg,
    slack,
    damp,
    scale,
    cache_o,
    read_o,
    G,
    Wf,
    Wv,
    Wq,
    Wg,
    X,
    SL,
    DM,
    SC,
    acc,
    U,
    LD,
    DS,
    PJ,
    KC,
    QC,
    NV,
    GT,
    RS_S,
    RS_R,
    TT,
    RD,
    CO,
    FO,
    tok_sem,
    in_sem,
    out_sem,
    ag_s,
    ag_r,
    rs_s,
    rs_r,
    tt_s,
    tt_r,
    rd_s,
    rd_r,
    pj_s,
    pj_r,
):
    NX, NSP, NQ, NH, LB, DB, HD, ROWS, SLAB = dims
    HALF = LB // 2
    CH = NH * HD
    gr = lax.axis_index("gr")
    sp = lax.axis_index("sp")
    tp = lax.axis_index("tp")
    x, c = tp // 2, tp % 2
    xl, xr, xo = (x + NX - 1) % NX, (x + 1) % NX, (x + 2) % NX
    sib = tp + 1 - 2 * c
    left, right, opp = 2 * xl + c, 2 * xr + c, 2 * xo + c
    left_s, right_s, opp_s = 2 * xl + 1 - c, 2 * xr + 1 - c, 2 * xo + 1 - c

    def tp_dev(t):
        return (gr, sp, t)

    def sp_dev(s):
        return (gr, s, tp)

    def tok_load(q):
        return pltpu.make_async_copy(tok.at[q], G.at[q, tp], tok_sem.at[q])

    loads = [
        pltpu.make_async_copy(src, dst, in_sem.at[i])
        for i, (src, dst) in enumerate(
            (
                (fti, X),
                (wq, Wq),
                (wg, Wg),
                (wf, Wf),
                (wv, Wv),
                (slack, SL),
                (damp, DM),
                (scale, SC),
            )
        )
    ]
    for q in range(NQ):
        tok_load(q).start()
    for copy in loads:
        copy.start()

    barrier = pltpu.get_barrier_semaphore()
    for t in (left, right, sib):
        pl.semaphore_signal(barrier, inc=1, device_id=tp_dev(t), device_id_type=MESH)

    def greet(k, carry):
        pl.semaphore_signal(
            barrier, inc=1, device_id=sp_dev((sp + k) % NSP), device_id_type=MESH
        )
        return carry

    lax.fori_loop(1, NSP, greet, 0)
    pl.semaphore_wait(barrier, 3 + NSP - 1)

    def ag(q, i, slot, part, dev):
        ref = G.at[q, slot]
        if part is not None:
            ref = G.at[q, slot, pl.ds(part * HALF, HALF)]
        return pltpu.make_async_remote_copy(
            src_ref=ref,
            dst_ref=ref,
            send_sem=ag_s.at[q, i],
            recv_sem=ag_r.at[q, i],
            device_id=tp_dev(dev),
            device_id_type=MESH,
        )

    def send_own(q):
        ag(q, 0, tp, None, right).start()
        ag(q, 1, tp, None, left).start()
        ag(q, 2, tp, None, sib).start()

    for q in range(AHEAD):
        tok_load(q).wait()
        send_own(q)

    for copy in loads[:5]:
        copy.wait()
    own_rows = pl.ds(sp * SLAB, SLAB)
    xv = X[...]

    def small(w):
        return jnp.dot(xv, w, preferred_element_type=F32)

    PJ[sp, 0:NQ, 0:CH] = small(Wq[...])
    PJ[sp, 0:NQ, CH : 2 * CH] = small(Wg[...])
    PJ[sp, NQ : 2 * NQ, 0:CH] = small(Wf[own_rows, :])
    PJ[sp, NQ : 2 * NQ, CH : 2 * CH] = small(Wv[own_rows, :])

    def spread(ref_of, ssem, rsem, peer):
        return pltpu.make_async_remote_copy(
            src_ref=ref_of(0),
            dst_ref=ref_of(1),
            send_sem=ssem,
            recv_sem=rsem,
            device_id=sp_dev(peer),
            device_id_type=MESH,
        )

    def pj_send(k, carry):
        p = (sp + k) % NSP
        spread(lambda _: PJ.at[sp], pj_s.at[p], pj_r.at[sp], p).start()
        return carry

    lax.fori_loop(1, NSP, pj_send, 0)

    for copy in loads[5:]:
        copy.wait()
    upper = lax.broadcasted_iota(jnp.int32, (LB, LB), 1) > lax.broadcasted_iota(
        jnp.int32, (LB, LB), 0
    )
    U[...] = jnp.where(upper, 1.0, 0.0).astype(BF16)

    def later_damping(q, carry):
        dq = DM[q]
        DS[q] = jnp.broadcast_to(jnp.sum(dq, axis=1, keepdims=True), (NH, HD))
        for h in range(NH):
            r = jnp.broadcast_to(dq[h : h + 1, :], (HD, LB))
            total = None
            for _ in range(3):
                part = r.astype(BF16)
                r = r - part.astype(F32)
                term = lax.dot_general(
                    U[...], part, (((1,), (1,)), ((), ())), preferred_element_type=F32
                )
                total = term if total is None else total + term
            LD[q, h] = total
        return carry

    lax.fori_loop(0, NQ, later_damping, 0)

    own_lane = (
        lax.broadcasted_iota(jnp.int32, (ROWS, HD), 1)
        == lax.broadcasted_iota(jnp.int32, (ROWS, HD), 0) + sp * ROWS
    )

    def own_column(row):
        picked = jnp.where(own_lane, jnp.broadcast_to(row, (ROWS, HD)), 0.0)
        return jnp.sum(picked, axis=1, keepdims=True)

    def multiply(q, par, xi, first):
        a0, a1 = G[q, 2 * xi], G[q, 2 * xi + 1]
        r0, r1 = pl.ds(xi * (2 * DB), DB), pl.ds(xi * (2 * DB) + DB, DB)
        for n, w in enumerate((Wf, Wv)):
            r = jnp.dot(a0, w[r0, :], preferred_element_type=F32)
            r += jnp.dot(a1, w[r1, :], preferred_element_type=F32)
            for h in range(NH):
                piece = r[:, h * HD : (h + 1) * HD]
                if first:
                    acc[par, n, h] = piece
                else:
                    acc[par, n, h] += piece

    def stage_a(q):
        par = q % 2
        ag(q, 2, sib, None, sib).wait_recv()
        multiply(q, par, x, True)
        ag(q, 0, left, None, left).wait_recv()
        ag(q, 5, left, 0, right).start()
        ag(q, 3, left, None, sib).start()
        ag(q, 1, right, None, right).wait_recv()
        ag(q, 6, right, 1, left).start()
        ag(q, 4, right, None, sib).start()

        @pl.when(q + AHEAD < NQ)
        def _():
            tok_load(q + AHEAD).wait()
            send_own(q + AHEAD)

        ag(q, 3, left_s, None, sib).wait_recv()
        multiply(q, par, xl, False)
        ag(q, 4, right_s, None, sib).wait_recv()
        multiply(q, par, xr, False)

    def rs_copy(q, p):
        return pltpu.make_async_remote_copy(
            src_ref=RS_S.at[q, p],
            dst_ref=RS_R.at[q, sp],
            send_sem=rs_s.at[q, p],
            recv_sem=rs_r.at[q, sp],
            device_id=sp_dev(p),
            device_id_type=MESH,
        )

    def tt_copy(q, p):
        return spread(lambda _: TT.at[q, sp], tt_s.at[q, p], tt_r.at[q, sp], p)

    def rd_copy(q, p):
        return spread(lambda _: RD.at[q, sp], rd_s.at[q, p], rd_r.at[q, sp], p)

    def stage_b(q):
        par = q % 2
        ag(q, 5, opp, 0, right).wait_recv()
        ag(q, 7, opp, 0, sib).start()
        ag(q, 6, opp, 1, left).wait_recv()
        ag(q, 8, opp, 1, sib).start()
        ag(q, 7, opp_s, 0, sib).wait_recv()
        ag(q, 8, opp_s, 1, sib).wait_recv()
        multiply(q, par, xo, False)
        totals, blocks = [], []
        for h in range(NH):
            f = acc[par, 0, h].astype(BF16).astype(F32)
            k = SL[h : h + 1, :] * jax.nn.sigmoid(-f)
            d = jnp.log1p(-k)
            d1 = d.astype(BF16)
            d2 = (d - d1.astype(F32)).astype(BF16)
            sums = jnp.dot(
                U[...], jnp.concatenate([d1, d2], axis=1), preferred_element_type=F32
            )
            later = sums[:, :HD] + sums[:, HD:] + LD[q, h]
            w = (k * jnp.exp(later)).astype(BF16)
            v = acc[par, 1, h].astype(BF16)
            s = lax.dot_general(w, v, (((0,), (0,)), ((), ())), preferred_element_type=F32)
            blocks.append(s.reshape(NSP, ROWS, HD))
            totals.append(jnp.sum(d, axis=0, keepdims=True))
        TT[q, sp] = jnp.concatenate(totals, axis=0) + DS[q]
        RS_S[q] = jnp.concatenate(blocks, axis=1).astype(BF16)

        def send(k, carry):
            p = (sp + k) % NSP
            tt_copy(q, p).start()
            rs_copy(q, p).start()
            return carry

        lax.fori_loop(1, NSP, send, 0)

    def wait_peers(copy_from):
        def wait(k, carry):
            copy_from((sp + k) % NSP).wait_recv()
            return carry

        lax.fori_loop(1, NSP, wait, 0)

    def from_peer(ref, rsem, ssem, p):
        return pltpu.make_async_remote_copy(
            src_ref=ref,
            dst_ref=ref,
            send_sem=ssem,
            recv_sem=rsem,
            device_id=sp_dev(p),
            device_id_type=MESH,
        )

    def new_token():
        wait_peers(lambda p: from_peer(PJ.at[p], pj_r.at[p], pj_s.at[p], p))
        total = PJ[0]
        for j in range(1, NSP):
            total = total + PJ[j]
        total = total.astype(BF16).astype(F32)
        GT[...] = total[0:NQ, CH : 2 * CH]
        for h in range(NH):
            lanes = slice(h * HD, (h + 1) * HD)
            qh = total[0:NQ, lanes]
            kh = SL[h : h + 1, :] * jax.nn.sigmoid(-total[NQ : 2 * NQ, lanes])
            vh = total[NQ : 2 * NQ, CH + h * HD : CH + (h + 1) * HD]
            for q in range(NQ):
                KC[q, h] = jnp.broadcast_to(own_column(kh[q : q + 1, :]), (ROWS, HD))
                QC[q, h] = jnp.broadcast_to(own_column(qh[q : q + 1, :]), (ROWS, HD))
                NV[q, h : h + 1, :] = vh[q : q + 1, :]

    def cache_out(q):
        return pltpu.make_async_copy(CO.at[q], cache_o.at[q], out_sem.at[q])

    def stage_c(q):
        wait_peers(lambda p: from_peer(TT.at[q, p], tt_r.at[q, p], tt_s.at[q, p], p))
        wait_peers(lambda p: from_peer(RS_R.at[q, p], rs_r.at[q, p], rs_s.at[q, p], p))
        RS_R[q, sp] = RS_S[q, sp]
        later = jnp.zeros((NH, HD), F32)
        sums = [jnp.zeros((ROWS, HD), F32) for _ in range(NH)]
        for j in reversed(range(NSP)):
            decay = jnp.exp(later)
            block = RS_R[q, j].astype(F32)
            for h in range(NH):
                sums[h] = sums[h] + own_column(decay[h : h + 1, :]) * block[
                    h * ROWS : (h + 1) * ROWS, :
                ]
            later = later + TT[q, j]
        parts = []
        for h in range(NH):
            kept = sums[h].astype(BF16)
            CO[q, h] = kept
            updated = (1.0 - KC[q, h]) * kept.astype(F32) + KC[q, h] * NV[q, h : h + 1, :]
            parts.append(jnp.sum(QC[q, h] * updated, axis=0, keepdims=True))
        RD[q, sp] = jnp.concatenate(parts, axis=0)

        def send(k, carry):
            rd_copy(q, (sp + k) % NSP).start()
            return carry

        lax.fori_loop(1, NSP, send, 0)
        cache_out(q).start()

    def step(it, carry):
        @pl.when(it < NQ)
        def _():
            stage_a(it)

        @pl.when(jnp.logical_and(it >= 1, it <= NQ))
        def _():
            stage_b(it - 1)

        @pl.when(it == 2)
        def _():
            new_token()

        @pl.when(it >= 2)
        def _():
            stage_c(it - 2)

        return carry

    lax.fori_loop(0, NQ + 2, step, 0)

    rows = []
    for q in range(NQ):
        wait_peers(lambda p: from_peer(RD.at[q, p], rd_r.at[q, p], rd_s.at[q, p], p))
        total = RD[q, 0]
        for j in range(1, NSP):
            total = total + RD[q, j]
        spread_of = jnp.mean(total * total, axis=-1, keepdims=True)
        scaled = total * lax.rsqrt(spread_of + 1e-06) * SC[...]
        rows.append(
            jnp.concatenate([scaled[h : h + 1, :] for h in range(NH)], axis=1)
        )
    FO[...] = (jnp.concatenate(rows, axis=0) * jax.nn.silu(GT[...])).astype(BF16)
    read_out = pltpu.make_async_copy(FO, read_o, out_sem.at[NQ])
    read_out.start()

    def drain_ag(q, carry):
        for i, part, dev in (
            (0, None, right),
            (1, None, left),
            (2, None, sib),
            (3, None, sib),
            (4, None, sib),
            (5, 0, right),
            (6, 1, left),
            (7, 0, sib),
            (8, 1, sib),
        ):
            ag(q, i, tp, part, dev).wait_send()
        cache_out(q).wait()

        def drain(k, inner):
            p = (sp + k) % NSP
            tt_copy(q, p).wait_send()
            rs_copy(q, p).wait_send()
            rd_copy(q, p).wait_send()
            return inner

        lax.fori_loop(1, NSP, drain, 0)
        return carry

    lax.fori_loop(0, NQ, drain_ag, 0)

    def drain_pj(k, carry):
        p = (sp + k) % NSP
        spread(lambda _: PJ.at[sp], pj_s.at[p], pj_r.at[sp], p).wait_send()
        return carry

    lax.fori_loop(1, NSP, drain_pj, 0)
    read_out.wait()


def per_device(tok, fti, wf, wv, wq, wg, slack, damp, scale):
    nq, lb, db = tok.shape
    hd = scale.shape[0]
    nh = damp.shape[2]
    nsp, ntp = lax.axis_size("sp"), lax.axis_size("tp")
    rows, slab, ch = hd // nsp, fti.shape[1], nh * hd
    dims = (ntp // 2, nsp, nq, nh, lb, db, hd, rows, slab)
    dma = pltpu.SemaphoreType.DMA
    V = pltpu.VMEM
    return pl.pallas_call(
        functools.partial(kernel, dims),
        out_shape=(
            jax.ShapeDtypeStruct((nq, nh, rows, hd), BF16),
            jax.ShapeDtypeStruct((nq, ch), BF16),
        ),
        in_specs=[pl.BlockSpec(memory_space=pl.ANY)] * 9,
        out_specs=[pl.BlockSpec(memory_space=pl.ANY)] * 2,
        scratch_shapes=[
            V((nq, ntp, lb, db), BF16),
            V(wf.shape, BF16),
            V(wv.shape, BF16),
            V(wq.shape, BF16),
            V(wg.shape, BF16),
            V(fti.shape, BF16),
            V((nh, hd), F32),
            V((nq, nh, lb), F32),
            V((1, hd), F32),
            V((2, 2, nh, lb, hd), F32),
            V((lb, lb), BF16),
            V((nq, nh, lb, hd), F32),
            V((nq, nh, hd), F32),
            V((nsp, 2 * nq, 2 * ch), F32),
            V((nq, nh, rows, hd), F32),
            V((nq, nh, rows, hd), F32),
            V((nq, nh, hd), F32),
            V((nq, ch), F32),
            V((nq, nsp, nh * rows, hd), BF16),
            V((nq, nsp, nh * rows, hd), BF16),
            V((nq, nsp, nh, hd), F32),
            V((nq, nsp, nh, hd), F32),
            V((nq, nh, rows, hd), BF16),
            V((nq, ch), BF16),
            dma((nq,)),
            dma((8,)),
            dma((nq + 1,)),
            dma((nq, 9)),
            dma((nq, 9)),
            dma((nq, nsp)),
            dma((nq, nsp)),
            dma((nq, nsp)),
            dma((nq, nsp)),
            dma((nq, nsp)),
            dma((nq, nsp)),
            dma((nsp,)),
            dma((nsp,)),
        ],
        compiler_params=pltpu.CompilerParams(
            collective_id=0, has_side_effects=True, vmem_limit_bytes=60 << 20
        ),
        name="linear_state",
    )(
        tok,
        fti,
        wf,
        wv,
        wq,
        wg,
        slack.reshape(nh, hd),
        jnp.swapaxes(damp, 1, 2),
        scale.reshape(1, hd),
    )


def solution(mesh):
    placed = (
        P("gr", "sp", "tp"),
        P("gr", "sp"),
        P(None, "tp"),
        P(None, "tp"),
        P("sp", "tp"),
        P("sp", "tp"),
        P("tp"),
        P("gr", "sp", "tp"),
        P(),
    )
    return jax.shard_map(
        per_device,
        mesh=mesh,
        in_specs=placed,
        out_specs=(P("gr", "tp", "sp", None), P("gr", "tp")),
        check_vma=False,
    )
```

```python
import functools

import jax
import jax.numpy as jnp
from jax import lax
from jax.experimental import pallas as pl
from jax.experimental.pallas import tpu as pltpu
from jax.sharding import PartitionSpec as P

MESH = pl.DeviceIdType.MESH
F32, BF16 = jnp.float32, jnp.bfloat16
AHEAD = 2


def kernel(
    dims,
    tok,
    fti,
    wf,
    wv,
    wq,
    wg,
    slack,
    damp,
    scale,
    cache_o,
    read_o,
    G,
    Wf,
    Wv,
    Wq,
    Wg,
    X,
    SL,
    DM,
    SC,
    acc,
    KS,
    DD,
    U,
    LD,
    DS,
    PJ,
    QK,
    CV,
    GT,
    SH,
    RS_S,
    RS_R,
    TT,
    RD,
    tok_sem,
    in_sem,
    ready,
    ag_s,
    ag_r,
    rs_s,
    rs_r,
    tt_s,
    tt_r,
    rd_s,
    rd_r,
    pj_s,
    pj_r,
):
    NX, NY, NZ, NQ, NH, LB, DB, HD, ROWS, SLAB = dims
    NSP = NY * NZ
    HALF = LB // 2
    CH = NH * HD
    gr = lax.axis_index("gr")
    sp = lax.axis_index("sp")
    tp = lax.axis_index("tp")
    x, c = tp // 2, tp % 2
    z, y = sp // NY, sp % NY
    xl, xr, xo = (x + NX - 1) % NX, (x + 1) % NX, (x + 2) % NX
    sib = tp + 1 - 2 * c
    left, right, opp = 2 * xl + c, 2 * xr + c, 2 * xo + c
    left_s, right_s, opp_s = 2 * xl + 1 - c, 2 * xr + 1 - c, 2 * xo + 1 - c

    def tp_dev(t):
        return (gr, sp, t)

    def sp_dev(s):
        return (gr, s, tp)

    def tok_load(q):
        return pltpu.make_async_copy(tok.at[q], G.at[q, tp], tok_sem.at[q])

    loads = [
        pltpu.make_async_copy(src, dst, in_sem.at[i])
        for i, (src, dst) in enumerate(
            (
                (fti, X),
                (wq, Wq),
                (wg, Wg),
                (wf, Wf),
                (wv, Wv),
                (slack, SL),
                (damp, DM),
                (scale, SC),
            )
        )
    ]

    def signal(sem, dev):
        pl.semaphore_signal(sem, inc=1, device_id=dev, device_id_type=MESH)

    def signal_y(sem):
        signal(sem, sp_dev(z * NY + (y + 1) % NY))
        signal(sem, sp_dev(z * NY + (y + NY - 1) % NY))

    def signal_z(sem):
        @pl.when(z > 0)
        def _():
            signal(sem, sp_dev(sp - NY))

        @pl.when(z < NZ - 1)
        def _():
            signal(sem, sp_dev(sp + NY))

    near_z = jnp.minimum(z, 1) + jnp.minimum(NZ - 1 - z, 1)

    barrier = pltpu.get_barrier_semaphore()
    for t in (left, right, sib):
        signal(barrier, tp_dev(t))
    signal_y(barrier)
    signal_z(barrier)
    for q in range(NQ):
        tok_load(q).start()
    for copy in loads:
        copy.start()
    pl.semaphore_wait(barrier, 5 + near_z)

    def ag(q, i, slot, part, dev):
        ref = G.at[q, slot]
        if part is not None:
            ref = G.at[q, slot, pl.ds(part * HALF, HALF)]
        return pltpu.make_async_remote_copy(
            src_ref=ref,
            dst_ref=ref,
            send_sem=ag_s.at[q, i],
            recv_sem=ag_r.at[q, i],
            device_id=tp_dev(dev),
            device_id_type=MESH,
        )

    def send_own(q):
        ag(q, 0, tp, None, right).start()
        ag(q, 1, tp, None, left).start()
        ag(q, 2, tp, None, sib).start()

    for q in range(AHEAD):
        tok_load(q).wait()
        send_own(q)

    signal_y(ready.at[0])

    for copy in loads[:5]:
        copy.wait()
    own_rows = pl.ds(sp * SLAB, SLAB)
    xv = X[...]

    def small(w):
        return jnp.dot(xv, w, preferred_element_type=F32)

    PJ[sp, 0:NQ, 0:CH] = small(Wq[...])
    PJ[sp, 0:NQ, CH : 2 * CH] = small(Wg[...])
    PJ[sp, NQ : 2 * NQ, 0:CH] = small(Wf[own_rows, :])
    PJ[sp, NQ : 2 * NQ, CH : 2 * CH] = small(Wv[own_rows, :])

    pl.semaphore_wait(ready.at[0], 2)
    signal_z(ready.at[1])

    for copy in loads[5:]:
        copy.wait()
    upper = lax.broadcasted_iota(jnp.int32, (LB, LB), 1) > lax.broadcasted_iota(
        jnp.int32, (LB, LB), 0
    )
    U[...] = jnp.where(upper, 1.0, 0.0).astype(BF16)
    for step in range(1, NZ - 1):
        pl.semaphore_wait(ready.at[step], near_z)
        signal_z(ready.at[step + 1])
    pl.semaphore_wait(ready.at[NZ - 1], near_z)

    def peers(copy_to):
        for k in range(NSP - 1):
            far = NSP // 2 + (k + 1) // 2 * (1 - 2 * (k % 2))
            copy_to((sp + far) % NSP).start()

    def spread(ref, ssem, rsem, peer):
        return pltpu.make_async_remote_copy(
            src_ref=ref,
            dst_ref=ref,
            send_sem=ssem,
            recv_sem=rsem,
            device_id=sp_dev(peer),
            device_id_type=MESH,
        )

    def all_blocks(ref, ssem, rsem):
        return spread(ref, ssem, rsem, (sp + 1) % NSP)

    def pj_copy(p):
        return spread(PJ.at[sp], pj_s, pj_r, p)

    pj_all = all_blocks(PJ.at[pl.ds(0, NSP - 1)], pj_s, pj_r)
    peers(pj_copy)

    def later_damping(q, carry):
        dq = DM[q]
        DS[q] = jnp.broadcast_to(jnp.sum(dq, axis=1, keepdims=True), (NH, HD))
        for h in range(NH):
            r = jnp.broadcast_to(dq[h : h + 1, :], (HD, LB))
            total = None
            for _ in range(3):
                part = r.astype(BF16)
                r = r - part.astype(F32)
                term = lax.dot_general(
                    U[...], part, (((1,), (1,)), ((), ())), preferred_element_type=F32
                )
                total = term if total is None else total + term
            LD[q, h] = total
        return carry

    lax.fori_loop(0, NQ, later_damping, 0)

    own_lane = (
        lax.broadcasted_iota(jnp.int32, (ROWS, HD), 1)
        == lax.broadcasted_iota(jnp.int32, (ROWS, HD), 0) + sp * ROWS
    )

    def own_column(row):
        picked = jnp.where(own_lane, jnp.broadcast_to(row, (ROWS, HD)), 0.0)
        return jnp.sum(picked, axis=1, keepdims=True)

    def multiply(q, par, xi, first, n):
        w = (Wf, Wv)[n]
        a0, a1 = G[q, 2 * xi], G[q, 2 * xi + 1]
        r0, r1 = pl.ds(xi * (2 * DB), DB), pl.ds(xi * (2 * DB) + DB, DB)
        r = jnp.dot(a0, w[r0, :], preferred_element_type=F32)
        r += jnp.dot(a1, w[r1, :], preferred_element_type=F32)
        for h in range(NH):
            piece = r[:, h * HD : (h + 1) * HD]
            if first:
                acc[par, n, h] = piece
            else:
                acc[par, n, h] += piece

    def stage_a(q):
        par = q % 2
        ag(q, 2, sib, None, sib).wait_recv()
        for n in (0, 1):
            multiply(q, par, x, True, n)
        ag(q, 0, left, None, left).wait_recv()
        ag(q, 5, left, 0, right).start()
        ag(q, 3, left, None, sib).start()
        ag(q, 1, right, None, right).wait_recv()
        ag(q, 6, right, 1, left).start()
        ag(q, 4, right, None, sib).start()

        @pl.when(q + AHEAD < NQ)
        def _():
            tok_load(q + AHEAD).wait()
            send_own(q + AHEAD)

        ag(q, 3, left_s, None, sib).wait_recv()
        for n in (0, 1):
            multiply(q, par, xl, False, n)
        ag(q, 4, right_s, None, sib).wait_recv()
        for n in (0, 1):
            multiply(q, par, xr, False, n)

    def rs_copy(q, p):
        return pltpu.make_async_remote_copy(
            src_ref=RS_S.at[q, p],
            dst_ref=RS_R.at[q, sp],
            send_sem=rs_s.at[q],
            recv_sem=rs_r.at[q],
            device_id=sp_dev(p),
            device_id_type=MESH,
        )

    def rs_all(q):
        return all_blocks(RS_R.at[q, pl.ds(0, NSP - 1)], rs_s.at[q], rs_r.at[q])

    def tt_copy(q, p):
        return spread(TT.at[q, sp], tt_s.at[q], tt_r.at[q], p)

    def tt_all(q):
        return all_blocks(TT.at[q, pl.ds(0, NSP - 1)], tt_s.at[q], tt_r.at[q])

    def rd_copy(q, p):
        return spread(RD.at[q, sp], rd_s.at[q], rd_r.at[q], p)

    def rd_all(q):
        return all_blocks(RD.at[q, pl.ds(0, NSP - 1)], rd_s.at[q], rd_r.at[q])

    def stage_b(q):
        par = q % 2
        ag(q, 5, opp, 0, right).wait_recv()
        ag(q, 7, opp, 0, sib).start()
        ag(q, 6, opp, 1, left).wait_recv()
        ag(q, 8, opp, 1, sib).start()
        ag(q, 7, opp_s, 0, sib).wait_recv()
        ag(q, 8, opp_s, 1, sib).wait_recv()
        multiply(q, par, xo, False, 0)
        totals = []
        for h in range(NH):
            f = acc[par, 0, h].astype(BF16).astype(F32)
            k = SL[h : h + 1, :] * jax.nn.sigmoid(-f)
            d = jnp.log1p(-k)
            d1 = d.astype(BF16)
            KS[h] = k
            DD[h, :, 0:HD] = d1
            DD[h, :, HD : 2 * HD] = (d - d1.astype(F32)).astype(BF16)
            totals.append(jnp.sum(d, axis=0, keepdims=True))
        TT[q, sp] = jnp.concatenate(totals, axis=0) + DS[q]
        peers(lambda p: tt_copy(q, p))
        multiply(q, par, xo, False, 1)
        blocks = []
        for h in range(NH):
            sums = jnp.dot(U[...], DD[h], preferred_element_type=F32)
            later = sums[:, :HD] + sums[:, HD:] + LD[q, h]
            w = (KS[h] * jnp.exp(later)).astype(BF16)
            v = acc[par, 1, h].astype(BF16)
            s = lax.dot_general(w, v, (((0,), (0,)), ((), ())), preferred_element_type=F32)
            SH[par, h * HD : (h + 1) * HD, :] = s.astype(BF16)
            blocks.append(s.reshape(NSP, ROWS, HD))
        RS_S[q] = jnp.concatenate(blocks, axis=1).astype(BF16)
        peers(lambda p: rs_copy(q, p))

    def new_token():
        pj_all.wait_recv()
        total = PJ[0]
        for j in range(1, NSP):
            total = total + PJ[j]
        total = total.astype(BF16).astype(F32)
        GT[...] = total[0:NQ, CH : 2 * CH]
        for q in range(NQ):

            def heads(row, start):
                return jnp.concatenate(
                    [
                        total[row : row + 1, start + h * HD : start + (h + 1) * HD]
                        for h in range(NH)
                    ],
                    axis=0,
                )

            query = heads(q, 0)
            keys = SL[...] * jax.nn.sigmoid(-heads(NQ + q, 0))
            QK[q] = query * (1.0 - keys)
            CV[q] = jnp.sum(query * keys, axis=1, keepdims=True) * heads(NQ + q, CH)

    def stage_r(q):
        par = q % 2
        tt_all(q).wait_recv()
        later = jnp.zeros((NH, HD), F32)
        for j in range(1, NSP):
            later = later + jnp.where(sp < j, TT[q, j], 0.0)
        coef = QK[q] * jnp.exp(later)
        high = coef.astype(BF16).astype(F32)
        both = jnp.concatenate([high, coef - high], axis=0)
        at_head = lax.broadcasted_iota(jnp.int32, (2 * NH, HD), 0) % NH
        spaced = jnp.concatenate(
            [jnp.where(at_head == h, both, 0.0) for h in range(NH)], axis=1
        ).astype(BF16)
        out = jnp.dot(spaced, SH[par], preferred_element_type=F32)
        RD[q, sp] = out[0:NH] + out[NH : 2 * NH]
        peers(lambda p: rd_copy(q, p))

    def stage_c(q):
        later = jnp.zeros((NH, HD), F32)
        columns = [None] * NSP
        for j in reversed(range(NSP)):
            decay = jnp.exp(later)
            columns[j] = [own_column(decay[h : h + 1, :]) for h in range(NH)]
            later = later + TT[q, j]
        rs_all(q).wait_recv()
        RS_R[q, sp] = RS_S[q, sp]
        sums = [jnp.zeros((ROWS, HD), F32) for _ in range(NH)]
        for j in reversed(range(NSP)):
            block = RS_R[q, j].astype(F32)
            for h in range(NH):
                sums[h] = sums[h] + columns[j][h] * block[h * ROWS : (h + 1) * ROWS, :]
        for h in range(NH):
            cache_o[q, h] = sums[h].astype(BF16)

    def step(it, carry):
        @pl.when(it < NQ)
        def _():
            stage_a(it)

        @pl.when(jnp.logical_and(it >= 1, it <= NQ))
        def _():
            stage_b(it - 1)

        @pl.when(it == 2)
        def _():
            new_token()

        @pl.when(jnp.logical_and(it >= 2, it <= NQ + 1))
        def _():
            stage_r(it - 2)

        @pl.when(it >= 3)
        def _():
            stage_c(it - 3)

        return carry

    lax.fori_loop(0, NQ + 3, step, 0)

    def drain(q, carry):
        for i, part in ((0, None), (1, None), (2, None), (3, None), (4, None)):
            ag(q, i, tp, part, sib).wait_send()
        for i, part in ((5, 0), (6, 1), (7, 0), (8, 1)):
            ag(q, i, tp, part, sib).wait_send()
        tt_all(q).wait_send()
        rs_all(q).wait_send()
        rd_all(q).wait_send()
        return carry

    lax.fori_loop(0, NQ, drain, 0)
    pj_all.wait_send()

    rows = []
    for q in range(NQ):
        rd_all(q).wait_recv()
        total = CV[q]
        for j in range(NSP):
            total = total + RD[q, j]
        spread_of = jnp.mean(total * total, axis=-1, keepdims=True)
        scaled = total * lax.rsqrt(spread_of + 1e-06) * SC[...]
        rows.append(
            jnp.concatenate([scaled[h : h + 1, :] for h in range(NH)], axis=1)
        )
    read_o[...] = (jnp.concatenate(rows, axis=0) * jax.nn.silu(GT[...])).astype(BF16)


def emit(cache, read, cache_o, read_o, sem):
    copies = [
        pltpu.make_async_copy(cache, cache_o, sem.at[0]),
        pltpu.make_async_copy(read, read_o, sem.at[1]),
    ]
    for copy in copies:
        copy.start()
    for copy in copies:
        copy.wait()


def per_device(tok, fti, wf, wv, wq, wg, slack, damp, scale):
    nq, lb, db = tok.shape
    hd = scale.shape[0]
    nh = damp.shape[2]
    nsp, ntp = lax.axis_size("sp"), lax.axis_size("tp")
    ny = 4
    nz = nsp // ny
    rows, slab, ch = hd // nsp, fti.shape[1], nh * hd
    dims = (ntp // 2, ny, nz, nq, nh, lb, db, hd, rows, slab)
    dma = pltpu.SemaphoreType.DMA
    V = pltpu.VMEM
    results = (
        jax.ShapeDtypeStruct((nq, nh, rows, hd), BF16),
        jax.ShapeDtypeStruct((nq, ch), BF16),
    )
    in_vmem = pl.BlockSpec(memory_space=pltpu.VMEM)
    outs = pl.pallas_call(
        functools.partial(kernel, dims),
        out_shape=tuple(V(r.shape, r.dtype) for r in results),
        in_specs=[pl.BlockSpec(memory_space=pl.ANY)] * 9,
        out_specs=[in_vmem] * 2,
        scratch_shapes=[
            V((nq, ntp, lb, db), BF16),
            V(wf.shape, BF16),
            V(wv.shape, BF16),
            V(wq.shape, BF16),
            V(wg.shape, BF16),
            V(fti.shape, BF16),
            V((nh, hd), F32),
            V((nq, nh, lb), F32),
            V((1, hd), F32),
            V((2, 2, nh, lb, hd), F32),
            V((nh, lb, hd), F32),
            V((nh, lb, 2 * hd), BF16),
            V((lb, lb), BF16),
            V((nq, nh, lb, hd), F32),
            V((nq, nh, hd), F32),
            V((nsp, 2 * nq, 2 * ch), F32),
            V((nq, nh, hd), F32),
            V((nq, nh, hd), F32),
            V((nq, ch), F32),
            V((2, nh * hd, hd), BF16),
            V((nq, nsp, nh * rows, hd), BF16),
            V((nq, nsp, nh * rows, hd), BF16),
            V((nq, nsp, nh, hd), F32),
            V((nq, nsp, nh, hd), F32),
            dma((nq,)),
            dma((8,)),
            pltpu.SemaphoreType.REGULAR((nz,)),
            dma((nq, 9)),
            dma((nq, 9)),
            dma((nq,)),
            dma((nq,)),
            dma((nq,)),
            dma((nq,)),
            dma((nq,)),
            dma((nq,)),
            dma,
            dma,
        ],
        compiler_params=pltpu.CompilerParams(
            collective_id=0, has_side_effects=True, vmem_limit_bytes=56 << 20
        ),
        name="linear_state",
    )(
        tok,
        fti,
        wf,
        wv,
        wq,
        wg,
        slack.reshape(nh, hd),
        jnp.swapaxes(damp, 1, 2),
        scale.reshape(1, hd),
    )
    return pl.pallas_call(
        emit,
        out_shape=results,
        in_specs=[in_vmem] * 2,
        out_specs=[pl.BlockSpec(memory_space=pl.ANY)] * 2,
        scratch_shapes=[dma((2,))],
        compiler_params=pltpu.CompilerParams(vmem_limit_bytes=4 << 20),
        name="emit",
    )(*outs)


def solution(mesh):
    placed = (
        P("gr", "sp", "tp"),
        P("gr", "sp"),
        P(None, "tp"),
        P(None, "tp"),
        P("sp", "tp"),
        P("sp", "tp"),
        P("tp"),
        P("gr", "sp", "tp"),
        P(),
    )
    return jax.shard_map(
        per_device,
        mesh=mesh,
        in_specs=placed,
        out_specs=(P("gr", "tp", "sp", None), P("gr", "tp")),
        check_vma=False,
    )
```

```python
import functools

import jax
import jax.numpy as jnp
from jax import lax
from jax.experimental import pallas as pl
from jax.experimental.pallas import tpu as pltpu
from jax.sharding import PartitionSpec as P

MESH = pl.DeviceIdType.MESH
F32, BF16 = jnp.float32, jnp.bfloat16


def kernel(
    dims,
    tok,
    fti,
    wf,
    wv,
    wq,
    wg,
    slack,
    damp,
    scale,
    cache_o,
    read_o,
    G,
    Wf,
    Wv,
    Wq,
    Wg,
    X,
    SL,
    DM,
    SC,
    acc,
    KS,
    DD,
    U,
    LD,
    DS,
    PJ,
    QK,
    CV,
    GT,
    SH,
    RS_S,
    RS_R,
    TT,
    RD,
    RW,
    tok_sem,
    in_sem,
    ready,
    ag_s,
    ag_r,
    rs_s,
    rs_r,
    tt_s,
    tt_r,
    rd_s,
    rd_r,
    pj_s,
    pj_r,
):
    NX, NY, NZ, NQ, NH, LB, DB, HD, ROWS, SLAB = dims
    NSP = NY * NZ
    HALF = LB // 2
    CH = NH * HD
    gr = lax.axis_index("gr")
    sp = lax.axis_index("sp")
    tp = lax.axis_index("tp")
    x, c = tp // 2, tp % 2
    z, y = sp // NY, sp % NY
    xl, xr, xo = (x + NX - 1) % NX, (x + 1) % NX, (x + 2) % NX
    sib = tp + 1 - 2 * c
    left, right, opp = 2 * xl + c, 2 * xr + c, 2 * xo + c
    left_s, right_s, opp_s = 2 * xl + 1 - c, 2 * xr + 1 - c, 2 * xo + 1 - c

    def tp_dev(t):
        return (gr, sp, t)

    def sp_dev(s):
        return (gr, s, tp)

    def tok_load(q):
        return pltpu.make_async_copy(tok.at[q], G.at[q, tp], tok_sem.at[q])

    loads = [
        pltpu.make_async_copy(src, dst, in_sem.at[i])
        for i, (src, dst) in enumerate(
            (
                (fti, X),
                (wq, Wq),
                (wg, Wg),
                (wf, Wf),
                (wv, Wv),
                (slack, SL),
                (damp, DM),
                (scale, SC),
            )
        )
    ]

    def signal(sem, dev):
        pl.semaphore_signal(sem, inc=1, device_id=dev, device_id_type=MESH)

    def signal_y(sem):
        signal(sem, sp_dev(z * NY + (y + 1) % NY))
        signal(sem, sp_dev(z * NY + (y + NY - 1) % NY))

    def signal_z(sem):
        @pl.when(z > 0)
        def _():
            signal(sem, sp_dev(sp - NY))

        @pl.when(z < NZ - 1)
        def _():
            signal(sem, sp_dev(sp + NY))

    near_z = jnp.minimum(z, 1) + jnp.minimum(NZ - 1 - z, 1)

    tok_load(0).start()
    barrier = pltpu.get_barrier_semaphore()
    for t in (left, right, sib):
        signal(barrier, tp_dev(t))
    signal_y(barrier)
    signal_z(barrier)
    tok_load(1).start()
    pl.semaphore_wait(barrier, 5 + near_z)

    def ag(q, i, slot, part, dev):
        ref = G.at[q, slot]
        if part is not None:
            ref = G.at[q, slot, pl.ds(part * HALF, HALF)]
        return pltpu.make_async_remote_copy(
            src_ref=ref,
            dst_ref=ref,
            send_sem=ag_s.at[q, i],
            recv_sem=ag_r.at[q, i],
            device_id=tp_dev(dev),
            device_id_type=MESH,
        )

    def send_first(q):
        ag(q, 0, tp, 0, right).start()
        ag(q, 1, tp, 1, left).start()
        ag(q, 2, tp, None, sib).start()

    def send_second(q):
        ag(q, 9, tp, 1, right).start()
        ag(q, 10, tp, 0, left).start()

    tok_load(0).wait()
    send_first(0)
    send_second(0)
    tok_load(1).wait()
    send_first(1)
    for copy in loads:
        copy.start()
    for q in range(2, NQ):
        tok_load(q).start()

    signal_y(ready.at[0])

    pl.semaphore_wait(ready.at[0], 2)
    signal_z(ready.at[1])

    upper = lax.broadcasted_iota(jnp.int32, (LB, LB), 1) > lax.broadcasted_iota(
        jnp.int32, (LB, LB), 0
    )
    U[...] = jnp.where(upper, 1.0, 0.0).astype(BF16)
    for step in range(1, NZ - 1):
        pl.semaphore_wait(ready.at[step], near_z)
        signal_z(ready.at[step + 1])
    pl.semaphore_wait(ready.at[NZ - 1], near_z)

    def peers(copy_to):
        for k in range(NSP - 1):
            far = NSP // 2 + (k + 1) // 2 * (1 - 2 * (k % 2))
            copy_to((sp + far) % NSP).start()

    def spread(ref, ssem, rsem, peer):
        return pltpu.make_async_remote_copy(
            src_ref=ref,
            dst_ref=ref,
            send_sem=ssem,
            recv_sem=rsem,
            device_id=sp_dev(peer),
            device_id_type=MESH,
        )

    def all_blocks(ref, ssem, rsem):
        return spread(ref, ssem, rsem, (sp + 1) % NSP)

    def pj_copy(p):
        return spread(PJ.at[sp], pj_s, pj_r, p)

    pj_all = all_blocks(PJ.at[pl.ds(0, NSP - 1)], pj_s, pj_r)
    def early():
        for copy in loads[:5]:
            copy.wait()
        own_rows = pl.ds(sp * SLAB, SLAB)
        xv = X[...]

        def small(w):
            return jnp.dot(xv, w, preferred_element_type=F32)

        PJ[sp, 0:NQ, 0:CH] = small(Wq[...])
        PJ[sp, 0:NQ, CH : 2 * CH] = small(Wg[...])
        PJ[sp, NQ : 2 * NQ, 0:CH] = small(Wf[own_rows, :])
        PJ[sp, NQ : 2 * NQ, CH : 2 * CH] = small(Wv[own_rows, :])

        peers(pj_copy)
        for copy in loads[5:]:
            copy.wait()

        def later_damping(q, carry):
            dq = DM[q]
            DS[q] = jnp.broadcast_to(jnp.sum(dq, axis=1, keepdims=True), (NH, HD))
            for h in range(NH):
                r = jnp.broadcast_to(dq[h : h + 1, :], (HD, LB))
                total = None
                for _ in range(3):
                    part = r.astype(BF16)
                    r = r - part.astype(F32)
                    term = lax.dot_general(
                        U[...], part, (((1,), (1,)), ((), ())), preferred_element_type=F32
                    )
                    total = term if total is None else total + term
                LD[q, h] = total
            return carry

        lax.fori_loop(0, NQ, later_damping, 0)

    own_lane = (
        lax.broadcasted_iota(jnp.int32, (ROWS, HD), 1)
        == lax.broadcasted_iota(jnp.int32, (ROWS, HD), 0) + sp * ROWS
    )

    def own_column(row):
        picked = jnp.where(own_lane, jnp.broadcast_to(row, (ROWS, HD)), 0.0)
        return jnp.sum(picked, axis=1, keepdims=True)

    def add_up(par, n, r, first):
        for h in range(NH):
            piece = r[:, h * HD : (h + 1) * HD]
            if first:
                acc[par, n, h] = piece
            else:
                acc[par, n, h] += piece

    def product(q, slot, n):
        rows = pl.ds(slot * DB, DB)
        return jnp.dot(G[q, slot], (Wf, Wv)[n][rows, :], preferred_element_type=F32)

    def multiply(q, par, xi, first):
        for n in (0, 1):
            add_up(par, n, product(q, 2 * xi, n) + product(q, 2 * xi + 1, n), first)

    def stage_a1(q):
        ag(q, 0, left, 0, left).wait_recv()
        ag(q, 5, left, 0, right).start()
        ag(q, 3, left, 0, sib).start()
        ag(q, 1, right, 1, right).wait_recv()
        ag(q, 6, right, 1, left).start()
        ag(q, 4, right, 1, sib).start()

        @pl.when(q + 1 < NQ)
        def _():
            send_second(q + 1)

        @pl.when(q + 2 < NQ)
        def _():
            tok_load(q + 2).wait()
            send_first(q + 2)

    def stage_own(q):
        ag(q, 2, sib, None, sib).wait_recv()
        multiply(q, q % 2, x, True)

    def stage_a2(q):
        ag(q, 9, left, 1, left).wait_recv()
        ag(q, 11, left, 1, sib).start()
        ag(q, 10, right, 0, right).wait_recv()
        ag(q, 12, right, 0, sib).start()
        ag(q, 3, left_s, 0, sib).wait_recv()
        ag(q, 11, left_s, 1, sib).wait_recv()
        multiply(q, q % 2, xl, False)
        ag(q, 4, right_s, 1, sib).wait_recv()
        ag(q, 12, right_s, 0, sib).wait_recv()
        multiply(q, q % 2, xr, False)

    def rs_copy(q, p):
        return pltpu.make_async_remote_copy(
            src_ref=RS_S.at[q, p],
            dst_ref=RS_R.at[q, sp],
            send_sem=rs_s.at[q],
            recv_sem=rs_r.at[q],
            device_id=sp_dev(p),
            device_id_type=MESH,
        )

    def rs_all(q):
        return all_blocks(RS_R.at[q, pl.ds(0, NSP - 1)], rs_s.at[q], rs_r.at[q])

    def tt_copy(q, p):
        return spread(TT.at[q, sp], tt_s.at[q], tt_r.at[q], p)

    def tt_all(q):
        return all_blocks(TT.at[q, pl.ds(0, NSP - 1)], tt_s.at[q], tt_r.at[q])

    def rd_copy(q, p):
        return spread(RD.at[q, sp], rd_s.at[q], rd_r.at[q], p)

    def rd_all(q):
        return all_blocks(RD.at[q, pl.ds(0, NSP - 1)], rd_s.at[q], rd_r.at[q])

    def stage_b(q):
        par = q % 2
        ag(q, 5, opp, 0, right).wait_recv()
        ag(q, 7, opp, 0, sib).start()
        ag(q, 6, opp, 1, left).wait_recv()
        ag(q, 8, opp, 1, sib).start()
        for n in (0, 1):
            add_up(par, n, product(q, opp, n), False)
        ag(q, 7, opp_s, 0, sib).wait_recv()
        ag(q, 8, opp_s, 1, sib).wait_recv()
        add_up(par, 0, product(q, opp_s, 0), False)
        totals = []
        for h in range(NH):
            f = acc[par, 0, h].astype(BF16).astype(F32)
            k = SL[h : h + 1, :] * jax.nn.sigmoid(-f)
            d = jnp.log1p(-k)
            d1 = d.astype(BF16)
            KS[h] = k
            DD[h, :, 0:HD] = d1
            DD[h, :, HD : 2 * HD] = (d - d1.astype(F32)).astype(BF16)
            totals.append(jnp.sum(d, axis=0, keepdims=True))
        TT[q, sp] = jnp.concatenate(totals, axis=0) + DS[q]
        peers(lambda p: tt_copy(q, p))
        add_up(par, 1, product(q, opp_s, 1), False)
        blocks = []
        for h in range(NH):
            sums = jnp.dot(U[...], DD[h], preferred_element_type=F32)
            later = sums[:, :HD] + sums[:, HD:] + LD[q, h]
            w = (KS[h] * jnp.exp(later)).astype(BF16)
            v = acc[par, 1, h].astype(BF16)
            s = lax.dot_general(w, v, (((0,), (0,)), ((), ())), preferred_element_type=F32)
            SH[par, h * HD : (h + 1) * HD, :] = s.astype(BF16)
            blocks.append(s.reshape(NSP, ROWS, HD))
        RS_S[q] = jnp.concatenate(blocks, axis=1).astype(BF16)
        peers(lambda p: rs_copy(q, p))

    def new_token():
        pj_all.wait_recv()
        total = PJ[0]
        for j in range(1, NSP):
            total = total + PJ[j]
        total = total.astype(BF16).astype(F32)
        GT[...] = total[0:NQ, CH : 2 * CH]
        for q in range(NQ):

            def heads(row, start):
                return jnp.concatenate(
                    [
                        total[row : row + 1, start + h * HD : start + (h + 1) * HD]
                        for h in range(NH)
                    ],
                    axis=0,
                )

            query = heads(q, 0)
            keys = SL[...] * jax.nn.sigmoid(-heads(NQ + q, 0))
            QK[q] = query * (1.0 - keys)
            CV[q] = jnp.sum(query * keys, axis=1, keepdims=True) * heads(NQ + q, CH)

    def stage_r(q):
        par = q % 2
        tt_all(q).wait_recv()
        later = jnp.zeros((NH, HD), F32)
        for j in range(1, NSP):
            later = later + jnp.where(sp < j, TT[q, j], 0.0)
        coef = QK[q] * jnp.exp(later)
        high = coef.astype(BF16).astype(F32)
        both = jnp.concatenate([high, coef - high], axis=0)
        at_head = lax.broadcasted_iota(jnp.int32, (2 * NH, HD), 0) % NH
        spaced = jnp.concatenate(
            [jnp.where(at_head == h, both, 0.0) for h in range(NH)], axis=1
        ).astype(BF16)
        out = jnp.dot(spaced, SH[par], preferred_element_type=F32)
        RD[q, sp] = out[0:NH] + out[NH : 2 * NH]
        peers(lambda p: rd_copy(q, p))

    def stage_c(q):
        later = jnp.zeros((NH, HD), F32)
        columns = [None] * NSP
        for j in reversed(range(NSP)):
            decay = jnp.exp(later)
            columns[j] = [own_column(decay[h : h + 1, :]) for h in range(NH)]
            later = later + TT[q, j]
        rs_all(q).wait_recv()
        RS_R[q, sp] = RS_S[q, sp]
        sums = [jnp.zeros((ROWS, HD), F32) for _ in range(NH)]
        for j in reversed(range(NSP)):
            block = RS_R[q, j].astype(F32)
            for h in range(NH):
                sums[h] = sums[h] + columns[j][h] * block[h * ROWS : (h + 1) * ROWS, :]
        for h in range(NH):
            cache_o[q, h] = sums[h].astype(BF16)

    def stage_d(q):
        rd_all(q).wait_recv()
        total = CV[q]
        for j in range(NSP):
            total = total + RD[q, j]
        spread_of = jnp.mean(total * total, axis=-1, keepdims=True)
        RW[q] = total * lax.rsqrt(spread_of + 1e-06) * SC[...]

    def drain(q, carry):
        for i, part in (
            (0, 0),
            (1, 1),
            (2, None),
            (3, 0),
            (4, 1),
            (5, 0),
            (6, 1),
            (7, 0),
            (8, 1),
            (9, 1),
            (10, 0),
            (11, 1),
            (12, 0),
        ):
            ag(q, i, tp, part, sib).wait_send()
        tt_all(q).wait_send()
        rs_all(q).wait_send()
        rd_all(q).wait_send()
        return carry

    def at(it, lag, stage):
        @pl.when(jnp.logical_and(it >= lag, it < NQ + lag))
        def _():
            stage(it - lag)

    def step(it, carry):
        at(it, 0, stage_a1)

        @pl.when(it == 0)
        def _():
            early()

        at(it, 0, stage_own)
        at(it, 1, stage_b)

        @pl.when(it == 2)
        def _():
            new_token()

        at(it, 2, stage_r)
        at(it, 4, stage_d)

        @pl.when(it == NQ + 2)
        def _():
            lax.fori_loop(0, NQ, drain, 0)
            pj_all.wait_send()

        at(it, 3, stage_c)
        at(it, 0, stage_a2)
        return carry

    lax.fori_loop(0, NQ + 4, step, 0)

    rows = [
        jnp.concatenate([RW[q, h : h + 1, :] for h in range(NH)], axis=1)
        for q in range(NQ)
    ]
    read_o[...] = (jnp.concatenate(rows, axis=0) * jax.nn.silu(GT[...])).astype(BF16)


def emit(cache, read, cache_o, read_o, sem):
    copies = [
        pltpu.make_async_copy(cache, cache_o, sem.at[0]),
        pltpu.make_async_copy(read, read_o, sem.at[1]),
    ]
    for copy in copies:
        copy.start()
    for copy in copies:
        copy.wait()


def per_device(tok, fti, wf, wv, wq, wg, slack, damp, scale):
    nq, lb, db = tok.shape
    hd = scale.shape[0]
    nh = damp.shape[2]
    nsp, ntp = lax.axis_size("sp"), lax.axis_size("tp")
    ny = 4
    nz = nsp // ny
    rows, slab, ch = hd // nsp, fti.shape[1], nh * hd
    dims = (ntp // 2, ny, nz, nq, nh, lb, db, hd, rows, slab)
    dma = pltpu.SemaphoreType.DMA
    V = pltpu.VMEM
    results = (
        jax.ShapeDtypeStruct((nq, nh, rows, hd), BF16),
        jax.ShapeDtypeStruct((nq, ch), BF16),
    )
    in_vmem = pl.BlockSpec(memory_space=pltpu.VMEM)
    outs = pl.pallas_call(
        functools.partial(kernel, dims),
        out_shape=tuple(V(r.shape, r.dtype) for r in results),
        in_specs=[pl.BlockSpec(memory_space=pl.ANY)] * 9,
        out_specs=[in_vmem] * 2,
        scratch_shapes=[
            V((nq, ntp, lb, db), BF16),
            V(wf.shape, BF16),
            V(wv.shape, BF16),
            V(wq.shape, BF16),
            V(wg.shape, BF16),
            V(fti.shape, BF16),
            V((nh, hd), F32),
            V((nq, nh, lb), F32),
            V((1, hd), F32),
            V((2, 2, nh, lb, hd), F32),
            V((nh, lb, hd), F32),
            V((nh, lb, 2 * hd), BF16),
            V((lb, lb), BF16),
            V((nq, nh, lb, hd), F32),
            V((nq, nh, hd), F32),
            V((nsp, 2 * nq, 2 * ch), F32),
            V((nq, nh, hd), F32),
            V((nq, nh, hd), F32),
            V((nq, ch), F32),
            V((2, nh * hd, hd), BF16),
            V((nq, nsp, nh * rows, hd), BF16),
            V((nq, nsp, nh * rows, hd), BF16),
            V((nq, nsp, nh, hd), F32),
            V((nq, nsp, nh, hd), F32),
            V((nq, nh, hd), F32),
            dma((nq,)),
            dma((8,)),
            pltpu.SemaphoreType.REGULAR((nz,)),
            dma((nq, 13)),
            dma((nq, 13)),
            dma((nq,)),
            dma((nq,)),
            dma((nq,)),
            dma((nq,)),
            dma((nq,)),
            dma((nq,)),
            dma,
            dma,
        ],
        compiler_params=pltpu.CompilerParams(
            collective_id=0, has_side_effects=True, vmem_limit_bytes=56 << 20
        ),
        name="linear_state",
    )(
        tok,
        fti,
        wf,
        wv,
        wq,
        wg,
        slack.reshape(nh, hd),
        jnp.swapaxes(damp, 1, 2),
        scale.reshape(1, hd),
    )
    return pl.pallas_call(
        emit,
        out_shape=results,
        in_specs=[in_vmem] * 2,
        out_specs=[pl.BlockSpec(memory_space=pl.ANY)] * 2,
        scratch_shapes=[dma((2,))],
        compiler_params=pltpu.CompilerParams(vmem_limit_bytes=4 << 20),
        name="emit",
    )(*outs)


def solution(mesh):
    placed = (
        P("gr", "sp", "tp"),
        P("gr", "sp"),
        P(None, "tp"),
        P(None, "tp"),
        P("sp", "tp"),
        P("sp", "tp"),
        P("tp"),
        P("gr", "sp", "tp"),
        P(),
    )
    return jax.shard_map(
        per_device,
        mesh=mesh,
        in_specs=placed,
        out_specs=(P("gr", "tp", "sp", None), P("gr", "tp")),
        check_vma=False,
    )
```

```python
import functools

import jax
import jax.numpy as jnp
from jax import lax
from jax.experimental import pallas as pl
from jax.experimental.pallas import tpu as pltpu
from jax.sharding import PartitionSpec as P

MESH = pl.DeviceIdType.MESH
F32, BF16 = jnp.float32, jnp.bfloat16


def kernel(
    dims,
    tok,
    fti,
    wf,
    wv,
    wq,
    wg,
    slack,
    damp,
    scale,
    cache_o,
    read_o,
    G,
    Wf,
    Wv,
    Wq,
    Wg,
    X,
    SL,
    DM,
    SC,
    acc,
    KS,
    DD,
    U,
    LD,
    DS,
    PJ,
    QK,
    CV,
    GT,
    SH,
    RS_S,
    RS_R,
    TT,
    RD,
    RW,
    tok_sem,
    in_sem,
    ready,
    ag_s,
    ag_r,
    rs_s,
    rs_r,
    tt_s,
    tt_r,
    rd_s,
    rd_r,
    pj_s,
    pj_r,
):
    NX, NY, NZ, NQ, NH, LB, DB, HD, ROWS, SLAB = dims
    NSP = NY * NZ
    HALF = LB // 2
    CH = NH * HD
    gr = lax.axis_index("gr")
    sp = lax.axis_index("sp")
    tp = lax.axis_index("tp")
    x, c = tp // 2, tp % 2
    z, y = sp // NY, sp % NY
    xl, xr, xo = (x + NX - 1) % NX, (x + 1) % NX, (x + 2) % NX
    sib = tp + 1 - 2 * c
    left, right, opp = 2 * xl + c, 2 * xr + c, 2 * xo + c
    left_s, right_s, opp_s = 2 * xl + 1 - c, 2 * xr + 1 - c, 2 * xo + 1 - c

    def tp_dev(t):
        return (gr, sp, t)

    def sp_dev(s):
        return (gr, s, tp)

    def tok_load(q):
        return pltpu.make_async_copy(tok.at[q], G.at[q, tp], tok_sem.at[q])

    loads = [
        pltpu.make_async_copy(src, dst, in_sem.at[i])
        for i, (src, dst) in enumerate(
            (
                (fti, X),
                (wq, Wq),
                (wg, Wg),
                (wf, Wf),
                (wv, Wv),
                (slack, SL),
                (damp, DM),
                (scale, SC),
            )
        )
    ]

    def signal(sem, dev):
        pl.semaphore_signal(sem, inc=1, device_id=dev, device_id_type=MESH)

    def signal_y(sem):
        signal(sem, sp_dev(z * NY + (y + 1) % NY))
        signal(sem, sp_dev(z * NY + (y + NY - 1) % NY))

    def signal_z(sem):
        @pl.when(z > 0)
        def _():
            signal(sem, sp_dev(sp - NY))

        @pl.when(z < NZ - 1)
        def _():
            signal(sem, sp_dev(sp + NY))

    near_z = jnp.minimum(z, 1) + jnp.minimum(NZ - 1 - z, 1)

    tok_load(0).start()
    barrier = pltpu.get_barrier_semaphore()
    for t in (left, right, sib):
        signal(barrier, tp_dev(t))
    signal_y(barrier)
    signal_z(barrier)
    tok_load(1).start()
    pl.semaphore_wait(barrier, 5 + near_z)

    def ag(q, i, slot, part, dev):
        ref = G.at[q, slot]
        if part is not None:
            ref = G.at[q, slot, pl.ds(part * HALF, HALF)]
        return pltpu.make_async_remote_copy(
            src_ref=ref,
            dst_ref=ref,
            send_sem=ag_s.at[q, i],
            recv_sem=ag_r.at[q, i],
            device_id=tp_dev(dev),
            device_id_type=MESH,
        )

    def send_first(q):
        ag(q, 0, tp, 0, right).start()
        ag(q, 1, tp, 1, left).start()
        ag(q, 2, tp, None, sib).start()

    def send_second(q):
        ag(q, 9, tp, 1, right).start()
        ag(q, 10, tp, 0, left).start()

    tok_load(0).wait()
    send_first(0)
    send_second(0)
    tok_load(1).wait()
    send_first(1)
    for copy in loads:
        copy.start()
    for q in range(2, NQ):
        tok_load(q).start()

    signal_y(ready.at[0])

    pl.semaphore_wait(ready.at[0], 2)
    signal_z(ready.at[1])

    upper = lax.broadcasted_iota(jnp.int32, (LB, LB), 1) > lax.broadcasted_iota(
        jnp.int32, (LB, LB), 0
    )
    U[...] = jnp.where(upper, 1.0, 0.0).astype(BF16)
    for step in range(1, NZ - 1):
        pl.semaphore_wait(ready.at[step], near_z)
        signal_z(ready.at[step + 1])
    pl.semaphore_wait(ready.at[NZ - 1], near_z)

    def peers(copy_to):
        for k in range(NSP - 1):
            far = NSP // 2 + (k + 1) // 2 * (1 - 2 * (k % 2))
            copy_to((sp + far) % NSP).start()

    def spread(ref, ssem, rsem, peer):
        return pltpu.make_async_remote_copy(
            src_ref=ref,
            dst_ref=ref,
            send_sem=ssem,
            recv_sem=rsem,
            device_id=sp_dev(peer),
            device_id_type=MESH,
        )

    def all_blocks(ref, ssem, rsem):
        return spread(ref, ssem, rsem, (sp + 1) % NSP)

    def pj_copy(p):
        return spread(PJ.at[sp], pj_s, pj_r, p)

    pj_all = all_blocks(PJ.at[pl.ds(0, NSP - 1)], pj_s, pj_r)
    def early():
        for copy in loads[:5]:
            copy.wait()
        own_rows = pl.ds(sp * SLAB, SLAB)
        xv = X[...]

        def small(w):
            return jnp.dot(xv, w, preferred_element_type=F32)

        PJ[sp, 0:NQ, 0:CH] = small(Wq[...])
        PJ[sp, 0:NQ, CH : 2 * CH] = small(Wg[...])
        PJ[sp, NQ : 2 * NQ, 0:CH] = small(Wf[own_rows, :])
        PJ[sp, NQ : 2 * NQ, CH : 2 * CH] = small(Wv[own_rows, :])

        peers(pj_copy)
        for copy in loads[5:]:
            copy.wait()

        def later_damping(q, carry):
            dq = DM[q]
            DS[q] = jnp.broadcast_to(jnp.sum(dq, axis=1, keepdims=True), (NH, HD))
            for h in range(NH):
                r = jnp.broadcast_to(dq[h : h + 1, :], (HD, LB))
                total = None
                for _ in range(3):
                    part = r.astype(BF16)
                    r = r - part.astype(F32)
                    term = lax.dot_general(
                        U[...], part, (((1,), (1,)), ((), ())), preferred_element_type=F32
                    )
                    total = term if total is None else total + term
                LD[q, h] = total
            return carry

        lax.fori_loop(0, NQ, later_damping, 0)

    own_lane = (
        lax.broadcasted_iota(jnp.int32, (ROWS, HD), 1)
        == lax.broadcasted_iota(jnp.int32, (ROWS, HD), 0) + sp * ROWS
    )

    def own_column(row):
        picked = jnp.where(own_lane, jnp.broadcast_to(row, (ROWS, HD)), 0.0)
        return jnp.sum(picked, axis=1, keepdims=True)

    def add_up(par, n, r, first):
        for h in range(NH):
            piece = r[:, h * HD : (h + 1) * HD]
            if first:
                acc[par, n, h] = piece
            else:
                acc[par, n, h] += piece

    def product(q, slot, n):
        rows = pl.ds(slot * DB, DB)
        return jnp.dot(G[q, slot], (Wf, Wv)[n][rows, :], preferred_element_type=F32)

    def stage_a1(q):
        ag(q, 0, left, 0, left).wait_recv()
        ag(q, 5, left, 0, right).start()
        ag(q, 3, left, 0, sib).start()
        ag(q, 1, right, 1, right).wait_recv()
        ag(q, 6, right, 1, left).start()
        ag(q, 4, right, 1, sib).start()

        @pl.when(q + 1 < NQ)
        def _():
            send_second(q + 1)

        @pl.when(q + 2 < NQ)
        def _():
            tok_load(q + 2).wait()
            send_first(q + 2)

    def stage_own(q):
        ag(q, 2, sib, None, sib).wait_recv()
        for n in (0, 1):
            add_up(q % 2, n, product(q, tp, n) + product(q, sib, n), True)

    def stage_a2(q):
        ag(q, 9, left, 1, left).wait_recv()
        ag(q, 11, left, 1, sib).start()
        ag(q, 10, right, 0, right).wait_recv()
        ag(q, 12, right, 0, sib).start()
        for n in (0, 1):
            add_up(q % 2, n, product(q, left, n) + product(q, right, n), False)
        ag(q, 3, left_s, 0, sib).wait_recv()
        ag(q, 11, left_s, 1, sib).wait_recv()
        ag(q, 4, right_s, 1, sib).wait_recv()
        ag(q, 12, right_s, 0, sib).wait_recv()
        for n in (0, 1):
            add_up(q % 2, n, product(q, left_s, n) + product(q, right_s, n), False)

    def rs_copy(q, p):
        return pltpu.make_async_remote_copy(
            src_ref=RS_S.at[q, p],
            dst_ref=RS_R.at[q, sp],
            send_sem=rs_s.at[q],
            recv_sem=rs_r.at[q],
            device_id=sp_dev(p),
            device_id_type=MESH,
        )

    def rs_all(q):
        return all_blocks(RS_R.at[q, pl.ds(0, NSP - 1)], rs_s.at[q], rs_r.at[q])

    def tt_copy(q, p):
        return spread(TT.at[q, sp], tt_s.at[q], tt_r.at[q], p)

    def tt_all(q):
        return all_blocks(TT.at[q, pl.ds(0, NSP - 1)], tt_s.at[q], tt_r.at[q])

    def rd_copy(q, p):
        return spread(RD.at[q, sp], rd_s.at[q], rd_r.at[q], p)

    def rd_all(q):
        return all_blocks(RD.at[q, pl.ds(0, NSP - 1)], rd_s.at[q], rd_r.at[q])

    def stage_b(q):
        par = q % 2
        ag(q, 5, opp, 0, right).wait_recv()
        ag(q, 7, opp, 0, sib).start()
        ag(q, 6, opp, 1, left).wait_recv()
        ag(q, 8, opp, 1, sib).start()
        for n in (0, 1):
            add_up(par, n, product(q, opp, n), False)
        ag(q, 7, opp_s, 0, sib).wait_recv()
        ag(q, 8, opp_s, 1, sib).wait_recv()
        add_up(par, 0, product(q, opp_s, 0), False)
        totals = []
        for h in range(NH):
            f = acc[par, 0, h].astype(BF16).astype(F32)
            k = SL[h : h + 1, :] * jax.nn.sigmoid(-f)
            d = jnp.log1p(-k)
            d1 = d.astype(BF16)
            KS[h] = k
            DD[h, :, 0:HD] = d1
            DD[h, :, HD : 2 * HD] = (d - d1.astype(F32)).astype(BF16)
            totals.append(jnp.sum(d, axis=0, keepdims=True))
        TT[q, sp] = jnp.concatenate(totals, axis=0) + DS[q]
        peers(lambda p: tt_copy(q, p))
        add_up(par, 1, product(q, opp_s, 1), False)
        blocks = []
        for h in range(NH):
            sums = jnp.dot(U[...], DD[h], preferred_element_type=F32)
            later = sums[:, :HD] + sums[:, HD:] + LD[q, h]
            w = (KS[h] * jnp.exp(later)).astype(BF16)
            v = acc[par, 1, h].astype(BF16)
            s = lax.dot_general(w, v, (((0,), (0,)), ((), ())), preferred_element_type=F32)
            SH[par, h * HD : (h + 1) * HD, :] = s.astype(BF16)
            blocks.append(s.reshape(NSP, ROWS, HD))
        RS_S[q] = jnp.concatenate(blocks, axis=1).astype(BF16)
        peers(lambda p: rs_copy(q, p))

    def new_token():
        pj_all.wait_recv()
        total = PJ[0]
        for j in range(1, NSP):
            total = total + PJ[j]
        total = total.astype(BF16).astype(F32)
        GT[...] = total[0:NQ, CH : 2 * CH]
        for q in range(NQ):

            def heads(row, start):
                return jnp.concatenate(
                    [
                        total[row : row + 1, start + h * HD : start + (h + 1) * HD]
                        for h in range(NH)
                    ],
                    axis=0,
                )

            query = heads(q, 0)
            keys = SL[...] * jax.nn.sigmoid(-heads(NQ + q, 0))
            QK[q] = query * (1.0 - keys)
            CV[q] = jnp.sum(query * keys, axis=1, keepdims=True) * heads(NQ + q, CH)

    def stage_r(q):
        par = q % 2
        tt_all(q).wait_recv()
        later = jnp.zeros((NH, HD), F32)
        for j in range(1, NSP):
            later = later + jnp.where(sp < j, TT[q, j], 0.0)
        coef = QK[q] * jnp.exp(later)
        high = coef.astype(BF16).astype(F32)
        both = jnp.concatenate([high, coef - high], axis=0)
        at_head = lax.broadcasted_iota(jnp.int32, (2 * NH, HD), 0) % NH
        spaced = jnp.concatenate(
            [jnp.where(at_head == h, both, 0.0) for h in range(NH)], axis=1
        ).astype(BF16)
        out = jnp.dot(spaced, SH[par], preferred_element_type=F32)
        RD[q, sp] = out[0:NH] + out[NH : 2 * NH]
        peers(lambda p: rd_copy(q, p))

    def stage_c(q):
        later = jnp.zeros((NH, HD), F32)
        columns = [None] * NSP
        for j in reversed(range(NSP)):
            decay = jnp.exp(later)
            columns[j] = [own_column(decay[h : h + 1, :]) for h in range(NH)]
            later = later + TT[q, j]
        rs_all(q).wait_recv()
        RS_R[q, sp] = RS_S[q, sp]
        sums = [jnp.zeros((ROWS, HD), F32) for _ in range(NH)]
        for j in reversed(range(NSP)):
            block = RS_R[q, j].astype(F32)
            for h in range(NH):
                sums[h] = sums[h] + columns[j][h] * block[h * ROWS : (h + 1) * ROWS, :]
        for h in range(NH):
            cache_o[q, h] = sums[h].astype(BF16)

    def stage_d(q):
        rd_all(q).wait_recv()
        total = CV[q]
        for j in range(NSP):
            total = total + RD[q, j]
        spread_of = jnp.mean(total * total, axis=-1, keepdims=True)
        RW[q] = total * lax.rsqrt(spread_of + 1e-06) * SC[...]

    def drain(q, carry):
        for i, part in (
            (0, 0),
            (1, 1),
            (2, None),
            (3, 0),
            (4, 1),
            (5, 0),
            (6, 1),
            (7, 0),
            (8, 1),
            (9, 1),
            (10, 0),
            (11, 1),
            (12, 0),
        ):
            ag(q, i, tp, part, sib).wait_send()
        tt_all(q).wait_send()
        rs_all(q).wait_send()
        rd_all(q).wait_send()
        return carry

    def at(it, lag, stage):
        @pl.when(jnp.logical_and(it >= lag, it < NQ + lag))
        def _():
            stage(it - lag)

    def step(it, carry):
        at(it, 0, stage_a1)

        @pl.when(it == 0)
        def _():
            early()

        at(it, 0, stage_own)
        at(it, 1, stage_b)

        @pl.when(it == 2)
        def _():
            new_token()

        at(it, 2, stage_r)
        at(it, 4, stage_d)

        @pl.when(it == NQ + 2)
        def _():
            lax.fori_loop(0, NQ, drain, 0)
            pj_all.wait_send()

        at(it, 3, stage_c)
        at(it, 0, stage_a2)
        return carry

    lax.fori_loop(0, NQ + 4, step, 0)

    rows = [
        jnp.concatenate([RW[q, h : h + 1, :] for h in range(NH)], axis=1)
        for q in range(NQ)
    ]
    read_o[...] = (jnp.concatenate(rows, axis=0) * jax.nn.silu(GT[...])).astype(BF16)


def emit(cache, read, cache_o, read_o, sem):
    copies = [
        pltpu.make_async_copy(cache, cache_o, sem.at[0]),
        pltpu.make_async_copy(read, read_o, sem.at[1]),
    ]
    for copy in copies:
        copy.start()
    for copy in copies:
        copy.wait()


def per_device(tok, fti, wf, wv, wq, wg, slack, damp, scale):
    nq, lb, db = tok.shape
    hd = scale.shape[0]
    nh = damp.shape[2]
    nsp, ntp = lax.axis_size("sp"), lax.axis_size("tp")
    ny = 4
    nz = nsp // ny
    rows, slab, ch = hd // nsp, fti.shape[1], nh * hd
    dims = (ntp // 2, ny, nz, nq, nh, lb, db, hd, rows, slab)
    dma = pltpu.SemaphoreType.DMA
    V = pltpu.VMEM
    results = (
        jax.ShapeDtypeStruct((nq, nh, rows, hd), BF16),
        jax.ShapeDtypeStruct((nq, ch), BF16),
    )
    in_vmem = pl.BlockSpec(memory_space=pltpu.VMEM)
    outs = pl.pallas_call(
        functools.partial(kernel, dims),
        out_shape=tuple(V(r.shape, r.dtype) for r in results),
        in_specs=[pl.BlockSpec(memory_space=pl.ANY)] * 9,
        out_specs=[in_vmem] * 2,
        scratch_shapes=[
            V((nq, ntp, lb, db), BF16),
            V(wf.shape, BF16),
            V(wv.shape, BF16),
            V(wq.shape, BF16),
            V(wg.shape, BF16),
            V(fti.shape, BF16),
            V((nh, hd), F32),
            V((nq, nh, lb), F32),
            V((1, hd), F32),
            V((2, 2, nh, lb, hd), F32),
            V((nh, lb, hd), F32),
            V((nh, lb, 2 * hd), BF16),
            V((lb, lb), BF16),
            V((nq, nh, lb, hd), F32),
            V((nq, nh, hd), F32),
            V((nsp, 2 * nq, 2 * ch), F32),
            V((nq, nh, hd), F32),
            V((nq, nh, hd), F32),
            V((nq, ch), F32),
            V((2, nh * hd, hd), BF16),
            V((nq, nsp, nh * rows, hd), BF16),
            V((nq, nsp, nh * rows, hd), BF16),
            V((nq, nsp, nh, hd), F32),
            V((nq, nsp, nh, hd), F32),
            V((nq, nh, hd), F32),
            dma((nq,)),
            dma((8,)),
            pltpu.SemaphoreType.REGULAR((nz,)),
            dma((nq, 13)),
            dma((nq, 13)),
            dma((nq,)),
            dma((nq,)),
            dma((nq,)),
            dma((nq,)),
            dma((nq,)),
            dma((nq,)),
            dma,
            dma,
        ],
        compiler_params=pltpu.CompilerParams(
            collective_id=0, has_side_effects=True, vmem_limit_bytes=56 << 20
        ),
        name="linear_state",
    )(
        tok,
        fti,
        wf,
        wv,
        wq,
        wg,
        slack.reshape(nh, hd),
        jnp.swapaxes(damp, 1, 2),
        scale.reshape(1, hd),
    )
    return pl.pallas_call(
        emit,
        out_shape=results,
        in_specs=[in_vmem] * 2,
        out_specs=[pl.BlockSpec(memory_space=pl.ANY)] * 2,
        scratch_shapes=[dma((2,))],
        compiler_params=pltpu.CompilerParams(vmem_limit_bytes=4 << 20),
        name="emit",
    )(*outs)


def solution(mesh):
    placed = (
        P("gr", "sp", "tp"),
        P("gr", "sp"),
        P(None, "tp"),
        P(None, "tp"),
        P("sp", "tp"),
        P("sp", "tp"),
        P("tp"),
        P("gr", "sp", "tp"),
        P(),
    )
    return jax.shard_map(
        per_device,
        mesh=mesh,
        in_specs=placed,
        out_specs=(P("gr", "tp", "sp", None), P("gr", "tp")),
        check_vma=False,
    )
```
